32 devices in a mesh: ra: 4 (over z), cb: 2 (over y), dp: 4 (over x, core).
Axes of the slice: x: 2, y: 2, z: 4, core: 2. Of those that a mesh axis runs over, the one named last changes fastest.
Arguments:
- tokens: bfloat16 [1792, 4096], P('dp', 'ra'), may hold values from -70 to 70
- norm_in: bfloat16 [4096], P('ra'), may hold values from 0.099609375 to 1.8984375
- w_up: float32 [4096, 16384], P(None, ('ra', 'cb')), may hold values from -0.09375 to 0.09375
- up_scale: float32 [16384], P(('ra', 'cb')), may hold values from 0.5 to 2
- w_down: float32 [16384, 4096], P('ra', 'cb'), may hold values from -0.0625 to 0.0625
- down_scale: float32 [4096], P('cb'), may hold values from 0.5 to 2
- norm_out: float32 [4096], P('cb'), may hold values from 0.1 to 1.9
Outputs:
- result: bfloat16 [1792, 4096], P('dp', 'cb')
The draws below stay inside these ranges and needn't reach their ends.
All inputs are finite; a program needn't handle non-finite values.
Results may differ from the reference program's by a relative error of at most 0.024.
Values may be sent and summed in bfloat16 or wider, within the bound.
A program may use at most 128 MiB of HBM per device.

```python
import math
import jax
import jax.numpy as jnp
from jax import lax

D = 4096
FF = 16384
TOKENS = 1792
N_RA = 4


def draw_tokens(key, part):
    key_base = jax.random.fold_in(key, 11)
    key_cols = jax.random.fold_in(key, 12)
    key_rows = jax.random.fold_in(key, 13)
    position = jnp.arange(D, dtype=jnp.float32) / D
    col_scale = jnp.exp(jnp.log(10.0) * (position - 0.5)) * jax.random.uniform(key_cols, (D,), jnp.float32, 0.7, 1.4)
    row_scale = jnp.exp(jax.random.uniform(key_rows, (TOKENS, 1), jnp.float32, jnp.log(0.3), jnp.log(3.0)))
    base = jnp.clip(jax.random.normal(key_base, (TOKENS, D), jnp.float32), -5.0, 5.0)
    return (base * col_scale[None, :] * row_scale).astype(jnp.bfloat16)


def with_spikes(array, rng, source, target, shards_of, factor):
    owner, partner = [(jnp.arange(array.shape[dim]) // (array.shape[dim] // shards_of)).reshape([-1 if axis == dim else 1 for axis in range(array.ndim)]) for dim in (source, target)]
    chosen = jax.random.permutation(rng, shards_of)[partner]
    strong = (owner == chosen) | (owner == (partner + shards_of // 2) % shards_of)
    return jnp.where(strong, factor * array, array)


def block_scale(own_key, extent, cuts, smallest, largest):
    loudness = 1.0
    for dim, shards_of in cuts:
        heights = jax.random.uniform(jax.random.fold_in(jax.random.fold_in(own_key, 6), dim), (shards_of,), jnp.float32, smallest / len(cuts), largest / len(cuts))
        loudness = loudness * jnp.repeat(jnp.exp(heights), extent[dim] // shards_of).reshape((-1,) + (1,) * (len(extent) - 1 - dim))
    return loudness


def scatter_about(own_key, extent, width, limit, shards=(), kind=jnp.bfloat16):
    result = jax.random.normal(own_key, extent, jnp.float32) * width
    if len(shards) > 0:
        result = block_scale(own_key, extent, shards, -0.22, 0.18) * result
    return jnp.clip(result, min=-limit, max=limit).astype(kind)


def bell_draw_with(key, shape, spread, limit, cuts, heavy, kind=jnp.bfloat16):
    drawn = spread * jax.random.normal(key, shape, jnp.float32)
    if cuts:
        drawn = drawn * block_scale(key, shape, cuts, -0.22, 0.18)
    return jnp.clip(with_spikes(drawn, jax.random.fold_in(key, 3), *heavy), -limit, limit).astype(kind)


def setup_inputs(seed: int = 0) -> dict:
    keys = jax.random.split(jax.random.key(seed), 8)
    tokens = draw_tokens(jax.random.fold_in(keys[7], 71), 0)
    norm_in = jnp.clip(1.0 + 0.18 * jax.random.normal(keys[1], (D,), jnp.float32), 0.099609375, 1.8984375).astype(jnp.bfloat16)
    w_up = scatter_about(keys[2], (D, FF), D ** -0.5, 0.09375, ((1, 8),), jnp.float32)
    up_scale = jnp.clip(jnp.exp(math.log(2.0) - 1.3862944 * jax.random.uniform(keys[3], (FF,), jnp.float32) ** block_scale(keys[3], (FF,), ((0, 8),), -0.2, 0.2)), 0.5, 2.0)
    w_down = bell_draw_with(keys[4], (FF, D), FF ** -0.5, 0.0625, ((0, 4), (1, 2)), (0, 1, 4, 2.0), jnp.float32)
    down_scale = jnp.clip(jnp.exp(math.log(2.0) - 1.3862944 * jax.random.uniform(keys[5], (D,), jnp.float32) ** block_scale(keys[5], (D,), ((0, 2),), -0.2, 0.2)), 0.5, 2.0)
    norm_out = jnp.clip(1.0 + 0.18 * jax.random.normal(keys[6], (D,), jnp.float32), 0.1, 1.9)
    return dict(tokens=tokens, norm_in=norm_in, w_up=w_up, up_scale=up_scale, w_down=w_down, down_scale=down_scale, norm_out=norm_out)


epsilon = 1e-06
resid_weight = 0.25

def reference(tokens, norm_in, w_up, up_scale, w_down, down_scale, norm_out):
    whole_float = tokens.astype(jnp.float32)
    inv_in = lax.rsqrt(lax.optimization_barrier(jnp.mean(whole_float * whole_float, axis=-1)) + epsilon)
    normed = (whole_float * norm_in.astype(jnp.float32)).astype(jnp.bfloat16)
    pre_act = jnp.dot(normed, w_up.astype(jnp.bfloat16), preferred_element_type=jnp.float32)
    pre_act = pre_act * inv_in[:, None] * up_scale
    hidden = jnp.square(jax.nn.relu(pre_act)).astype(jnp.bfloat16)
    block_rows = FF // N_RA
    weight_blocks = w_down.astype(jnp.bfloat16).reshape(N_RA, block_rows, D)
    hidden_blocks = hidden.reshape(hidden.shape[0], N_RA, block_rows).transpose(1, 0, 2)

    def add_block(total, pair):
        hidden_part, weight_part = pair
        part = jnp.dot(hidden_part, weight_part, preferred_element_type=jnp.float32).astype(jnp.bfloat16)
        part = lax.optimization_barrier(part)
        return (total + part.astype(jnp.float32), None)
    start_total = jnp.zeros((hidden.shape[0], D), jnp.float32)
    down, _ = lax.scan(add_block, start_total, (hidden_blocks, weight_blocks))
    mixed = resid_weight * whole_float + down * down_scale
    inv_out = lax.rsqrt(lax.optimization_barrier(jnp.mean(mixed * mixed, axis=-1)) + epsilon)
    return (mixed * inv_out[:, None] * norm_out).astype(jnp.bfloat16)
```

```python
import functools

import jax
import jax.numpy as jnp
from jax import lax
from jax.experimental import pallas as pl
from jax.experimental.pallas import tpu as pltpu
from jax.sharding import PartitionSpec as P

epsilon = 1e-06
resid_weight = 0.25
MESH = pl.DeviceIdType.MESH
CHUNKS = 4
SLOTS = 6
STEP_ROWS = 128


def plain(tokens, norm_in, w_up, up_scale, w_down, down_scale, norm_out):
    whole_rows, whole_gain = (
        lax.all_gather(tokens, "ra", axis=1, tiled=True),
        lax.all_gather(norm_in, "ra", axis=0, tiled=True),
    )
    whole_float = whole_rows.astype(jnp.float32)
    model_width = whole_float.shape[1]
    inv_in = lax.rsqrt(jnp.mean(whole_float * whole_float, axis=-1) + epsilon)
    normed = (whole_float * whole_gain.astype(jnp.float32)).astype(jnp.bfloat16)
    pre_act = jnp.dot(normed, w_up.astype(jnp.bfloat16), preferred_element_type=jnp.float32)
    pre_act = pre_act * inv_in[:, None] * up_scale
    hidden = jnp.square(jax.nn.relu(pre_act)).astype(jnp.bfloat16)
    down_bf = w_down.astype(jnp.bfloat16)
    quarter = down_bf.shape[1]
    partial_value = jnp.dot(
        lax.all_gather(hidden, "cb", axis=1, tiled=True),
        down_bf,
        preferred_element_type=jnp.float32,
    )
    col_block = lax.axis_index("cb")
    x_quarter = lax.dynamic_slice_in_dim(whole_float, col_block * quarter, quarter, 1)
    down = lax.psum(partial_value.astype(jnp.bfloat16), "ra").astype(jnp.float32)
    mixed = resid_weight * x_quarter + down * down_scale
    total_sq = lax.psum(jnp.sum(mixed * mixed, axis=-1), "cb")
    inv_out = lax.rsqrt(total_sq / model_width + epsilon)
    return (mixed * inv_out[:, None] * norm_out).astype(jnp.bfloat16)


def kernel(
    n, chunks,
    x_ref, gain_ref, wu_ref, us_ref, wd_ref, ds_ref, no_ref,
    o_ref,
    xa, gains, wu, wd, stage, normed, hid, parts, rbuf, down, mixed, sq, sqr,
    load_sem, own_sem, gs, gr,
    xs, xr, ys, yr, hs, hr, rs, rr, fs, fr, qs, qr,
):
    z = lax.axis_index("ra")
    y = lax.axis_index("cb")
    twin = 1 - y
    rows = xa.shape[3]
    half = xa.shape[4]
    model_width = 2 * n * half
    up_cols = wu.shape[1]
    steps = wu.shape[0] // STEP_ROWS

    def load(ref, i, slot):
        return pltpu.make_async_copy(
            ref.at[pl.ds(i * STEP_ROWS, STEP_ROWS)], stage.at[slot], load_sem.at[slot]
        )

    for i in range(SLOTS):
        load(wu_ref, i, i).start()

    def own_piece(c, h):
        return pltpu.make_async_copy(
            x_ref.at[pl.ds(c * rows, rows), pl.ds(h * half, half)],
            xa.at[c, z, h],
            own_sem.at[c, h],
        )

    for c in range(chunks):
        for h in range(2):
            own_piece(c, h).start()

    barrier = pltpu.get_barrier_semaphore()
    for j in range(1, n):
        pl.semaphore_signal(
            barrier, inc=1, device_id={"ra": lax.rem(z + j, n)}, device_id_type=MESH
        )
    pl.semaphore_signal(barrier, inc=1, device_id={"cb": twin}, device_id_type=MESH)
    pl.semaphore_wait(barrier, n)

    def remote(src, dst, send, recv, where):
        return pltpu.make_async_remote_copy(
            src_ref=src, dst_ref=dst, send_sem=send, recv_sem=recv,
            device_id=where, device_id_type=MESH,
        )

    def x_copy(c, src, way):
        piece = xa.at[c, src, y]
        return remote(piece, piece, xs.at[c, src, way], xr.at[c, src], {"ra": z + 1 - 2 * way})

    def y_copy(c, src):
        piece = xa.at[c, src, y]
        return remote(piece, piece, ys.at[c, src], yr.at[c, src], {"cb": twin})

    def y_arrive(c, src):
        piece = xa.at[c, src, twin]
        return remote(piece, piece, ys.at[c, src], yr.at[c, src], {"cb": twin})

    def d_copy(c, src, way):
        piece = down.at[c, src]
        return remote(piece, piece, fs.at[c, src, way], fr.at[c, src], {"ra": z + 1 - 2 * way})

    def start_line(copy, c):
        @pl.when(z + 1 < n)
        def _():
            copy(c, z, 0).start()

        @pl.when(z > 0)
        def _():
            copy(c, z, 1).start()

    def relay(copy, c, k, also=None):
        @pl.when(z - k >= 0)
        def _():
            src = z - k
            copy(c, src, 0).wait_recv()

            @pl.when(z + 1 < n)
            def _():
                copy(c, src, 0).start()

            if also is not None:
                also(c, src).start()

        @pl.when(z + k < n)
        def _():
            src = z + k
            copy(c, src, 1).wait_recv()

            @pl.when(z > 0)
            def _():
                copy(c, src, 1).start()

            if also is not None:
                also(c, src).start()

    def gain_copy(where, src):
        return remote(gain_ref, gains.at[src], gs.at[where], gr.at[src], {"ra": where})

    def begin(c):
        if c < chunks:
            for h in range(2):
                own_piece(c, h).wait()
            start_line(x_copy, c)

    begin(0)
    for j in range(1, n):
        gain_copy(lax.rem(z + j, n), z).start()
    gains[z] = gain_ref[...]
    begin(1)

    def gather_step(c, k):
        relay(x_copy, c, k, y_copy)
        if k == 1:
            begin(c + 2)

    def convert(ref, target, following, lo, hi):
        def body(i, carry):
            slot = lax.rem(i + (0 if following is not None else steps), SLOTS)
            load(ref, i, slot).wait()
            target[pl.ds(pl.multiple_of(i * STEP_ROWS, STEP_ROWS), STEP_ROWS), :] = stage[
                slot
            ].astype(jnp.bfloat16)

            @pl.when(i + SLOTS < steps)
            def _():
                load(ref, i + SLOTS, slot).start()

            if following is not None:
                @pl.when(i + SLOTS >= steps)
                def _():
                    load(following, i + SLOTS - steps, slot).start()

            return carry

        lax.fori_loop(lo, hi, body, 0)

    def convert_with_gather(ref, target, following, c):
        cuts = [steps * k // n for k in range(n + 1)]
        for k in range(1, n + 1):
            convert(ref, target, following, cuts[k - 1], cuts[k])
            if k < n and c < chunks:
                gather_step(c, k)

    def hid_copy(c, block):
        piece = hid.at[c, block]
        return remote(piece, piece, hs.at[c], hr.at[c], {"cb": twin})

    def up(c):
        for j in range(1, n):
            y_arrive(c, lax.rem(z + j, n)).wait_recv()
        total = jnp.zeros((rows, 1), jnp.float32)
        for s in range(n):
            for h in range(2):
                xf = xa[c, s, h].astype(jnp.float32)
                total += jnp.sum(xf * xf, axis=1, keepdims=True)
                gain = gains[s][:, h * half : (h + 1) * half]
                lo = (2 * s + h) * half
                normed[:, lo : lo + half] = (xf * gain).astype(jnp.bfloat16)
        inv_in = lax.rsqrt(total / model_width + epsilon)
        tile = 256

        def body(j, carry):
            cols = pl.ds(pl.multiple_of(j * tile, tile), tile)
            pre = jnp.dot(normed[...], wu[:, cols], preferred_element_type=jnp.float32)
            pre = jnp.maximum(pre * inv_in * us_ref[:, cols], 0.0)
            hid[c, y, :, cols] = (pre * pre).astype(jnp.bfloat16)
            return carry

        lax.fori_loop(0, up_cols // tile, body, 0)
        hid_copy(c, y).start()

    def part_copy(c, where, src):
        return remote(
            parts.at[c, where], rbuf.at[c, src], rs.at[c, where], rr.at[c, src], {"ra": where}
        )

    def down_product(c):
        hid_copy(c, twin).wait_recv()

        def body(q, carry):
            cols = pl.ds(pl.multiple_of(q * half, half), half)
            acc = jnp.dot(hid[c, 0], wd[:up_cols, cols], preferred_element_type=jnp.float32)
            acc += jnp.dot(hid[c, 1], wd[up_cols:, cols], preferred_element_type=jnp.float32)
            parts[c, q] = acc.astype(jnp.bfloat16)
            return carry

        lax.fori_loop(0, n, body, 0)
        for j in range(1, n):
            part_copy(c, lax.rem(z + j, n), z).start()

    def reduce(c):
        acc = parts[c, z].astype(jnp.float32)
        for j in range(1, n):
            src = lax.rem(z + j, n)
            part_copy(c, src, src).wait_recv()
            acc += rbuf[c, src].astype(jnp.float32)
        down[c, z] = acc.astype(jnp.bfloat16)
        start_line(d_copy, c)

    def sq_copy(c):
        return remote(sq.at[c], sqr.at[c], qs.at[c], qr.at[c], {"cb": twin})

    def mix(c):
        for k in range(1, n):
            relay(d_copy, c, k)
        total = jnp.zeros((rows, 1), jnp.float32)
        for q in range(n):
            cols = slice(q * half, (q + 1) * half)
            at = y * n + q
            resid = xa[c, at // 2, at % 2].astype(jnp.float32)
            value = resid_weight * resid + down[c, q].astype(jnp.float32) * ds_ref[:, cols]
            mixed[c % 2, :, cols] = value
            total += jnp.sum(value * value, axis=1, keepdims=True)
        sq[c] = jnp.broadcast_to(total, (rows, 128))
        sq_copy(c).start()

    def finish(c):
        sq_copy(c).wait_recv()
        total = sq[c][:, :1] + sqr[c][:, :1]
        inv_out = lax.rsqrt(total / model_width + epsilon)
        o_ref[c * rows : (c + 1) * rows, :] = (mixed[c % 2] * inv_out * no_ref[...]).astype(
            jnp.bfloat16
        )

    convert_with_gather(wu_ref, wu, wd_ref, 0)
    for j in range(1, n):
        src = lax.rem(z + j, n)
        gain_copy(src, src).wait_recv()
    up(0)
    convert_with_gather(wd_ref, wd, None, 1)
    for t in range(1, chunks + 4):
        if t < chunks:
            if t > 1:
                for k in range(1, n):
                    gather_step(t, k)
            up(t)
        if 0 <= t - 1 < chunks:
            down_product(t - 1)
        if 0 <= t - 2 < chunks:
            reduce(t - 2)
        if 0 <= t - 4 < chunks:
            finish(t - 4)
        if 0 <= t - 3 < chunks:
            mix(t - 3)

    for j in range(1, n):
        gain_copy(lax.rem(z + j, n), z).wait_send()

    def drain(c, carry):
        for src in range(n):
            @pl.when((src <= z) & (z + 1 < n))
            def _():
                x_copy(c, src, 0).wait_send()
                d_copy(c, src, 0).wait_send()

            @pl.when((src >= z) & (z > 0))
            def _():
                x_copy(c, src, 1).wait_send()
                d_copy(c, src, 1).wait_send()

            @pl.when(z != src)
            def _():
                y_copy(c, src).wait_send()
                part_copy(c, src, z).wait_send()

        hid_copy(c, y).wait_send()
        sq_copy(c).wait_send()
        return carry

    lax.fori_loop(0, chunks, drain, 0)


def fused(n, tokens, norm_in, w_up, up_scale, w_down, down_scale, norm_out):
    chunks = CHUNKS
    rows = tokens.shape[0] // chunks
    half = tokens.shape[1] // 2
    wide = w_down.shape[1]
    bf16, f32 = jnp.bfloat16, jnp.float32
    dma = pltpu.SemaphoreType.DMA
    vmem = pl.BlockSpec(memory_space=pltpu.VMEM)
    far = pl.BlockSpec(memory_space=pl.ANY)
    flops = 2 * tokens.shape[0] * (w_up.size + w_down.size)
    return pl.pallas_call(
        functools.partial(kernel, n, chunks),
        out_shape=jax.ShapeDtypeStruct((tokens.shape[0], wide), bf16),
        in_specs=[far, vmem, far, vmem, far, vmem, vmem],
        out_specs=vmem,
        scratch_shapes=[
            pltpu.VMEM((chunks, n, 2, rows, half), bf16),
            pltpu.VMEM((n, 1, 2 * half), f32),
            pltpu.VMEM(w_up.shape, bf16),
            pltpu.VMEM(w_down.shape, bf16),
            pltpu.VMEM((SLOTS, STEP_ROWS, wide), f32),
            pltpu.VMEM((rows, 2 * half * n), bf16),
            pltpu.VMEM((chunks, 2, rows, w_up.shape[1]), bf16),
            pltpu.VMEM((chunks, n, rows, half), bf16),
            pltpu.VMEM((chunks, n, rows, half), bf16),
            pltpu.VMEM((chunks, n, rows, half), bf16),
            pltpu.VMEM((2, rows, wide), f32),
            pltpu.VMEM((chunks, rows, 128), f32),
            pltpu.VMEM((chunks, rows, 128), f32),
            dma((SLOTS,)),
            dma((chunks, 2)),
            dma((n,)),
            dma((n,)),
            dma((chunks, n, 2)),
            dma((chunks, n)),
            dma((chunks, n)),
            dma((chunks, n)),
            dma((chunks,)),
            dma((chunks,)),
            dma((chunks, n)),
            dma((chunks, n)),
            dma((chunks, n, 2)),
            dma((chunks, n)),
            dma((chunks,)),
            dma((chunks,)),
        ],
        compiler_params=pltpu.CompilerParams(
            collective_id=0, has_side_effects=True, vmem_limit_bytes=67043328
        ),
        cost_estimate=pl.CostEstimate(
            flops=flops, bytes_accessed=4 * (w_up.size + w_down.size), transcendentals=0
        ),
    )(
        tokens,
        norm_in.astype(f32)[None, :],
        w_up,
        up_scale[None, :],
        w_down,
        down_scale[None, :],
        norm_out[None, :],
    )


def solution(mesh):
    n, m = mesh.shape["ra"], mesh.shape["cb"]

    def per_device(tokens, norm_in, w_up, up_scale, w_down, down_scale, norm_out):
        args = (tokens, norm_in, w_up, up_scale, w_down, down_scale, norm_out)
        fits = (
            m == 2
            and n > 1
            and CHUNKS > 1
            and tokens.shape[0] % (CHUNKS * 16) == 0
            and tokens.shape[1] % 256 == 0
            and w_up.shape == w_down.shape
            and w_up.shape[0] % (STEP_ROWS * n) == 0
            and w_up.shape[0] // STEP_ROWS >= SLOTS
            and w_up.shape[1] % 256 == 0
            and w_up.size <= 8 * 1024 * 1024
            and tokens.size * n <= 2 * 1024 * 1024
        )
        return fused(n, *args) if fits else plain(*args)

    placed = (
        P("dp", "ra"),
        P("ra"),
        P(None, ("ra", "cb")),
        P(("ra", "cb")),
        P("ra", "cb"),
        P("cb"),
        P("cb"),
    )
    return jax.shard_map(
        per_device, mesh=mesh, in_specs=placed, out_specs=P("dp", "cb"), check_vma=False
    )
```

```python
import functools

import jax
import jax.numpy as jnp
from jax import lax
from jax.experimental import pallas as pl
from jax.experimental.pallas import tpu as pltpu
from jax.sharding import PartitionSpec as P

epsilon = 1e-06
resid_weight = 0.25
MESH = pl.DeviceIdType.MESH
CHUNKS = 4
SLOTS = 6
STEP_ROWS = 128


def plain(tokens, norm_in, w_up, up_scale, w_down, down_scale, norm_out):
    whole_rows, whole_gain = (
        lax.all_gather(tokens, "ra", axis=1, tiled=True),
        lax.all_gather(norm_in, "ra", axis=0, tiled=True),
    )
    whole_float = whole_rows.astype(jnp.float32)
    model_width = whole_float.shape[1]
    inv_in = lax.rsqrt(jnp.mean(whole_float * whole_float, axis=-1) + epsilon)
    normed = (whole_float * whole_gain.astype(jnp.float32)).astype(jnp.bfloat16)
    pre_act = jnp.dot(normed, w_up.astype(jnp.bfloat16), preferred_element_type=jnp.float32)
    pre_act = pre_act * inv_in[:, None] * up_scale
    hidden = jnp.square(jax.nn.relu(pre_act)).astype(jnp.bfloat16)
    down_bf = w_down.astype(jnp.bfloat16)
    quarter = down_bf.shape[1]
    partial_value = jnp.dot(
        lax.all_gather(hidden, "cb", axis=1, tiled=True),
        down_bf,
        preferred_element_type=jnp.float32,
    )
    col_block = lax.axis_index("cb")
    x_quarter = lax.dynamic_slice_in_dim(whole_float, col_block * quarter, quarter, 1)
    down = lax.psum(partial_value.astype(jnp.bfloat16), "ra").astype(jnp.float32)
    mixed = resid_weight * x_quarter + down * down_scale
    total_sq = lax.psum(jnp.sum(mixed * mixed, axis=-1), "cb")
    inv_out = lax.rsqrt(total_sq / model_width + epsilon)
    return (mixed * inv_out[:, None] * norm_out).astype(jnp.bfloat16)


def kernel(
    n, chunks,
    x_ref, gain_ref, wu_ref, us_ref, wd_ref, ds_ref, no_ref,
    o_ref,
    xa, gains, wu, wd, stage, normed, hid, parts, rbuf, down, mixed, sq, sqr,
    load_sem, own_sem, gs, gr,
    xs, xr, ys, yr, hs, hr, rs, rr, fs, fr, qs, qr,
):
    z = lax.axis_index("ra")
    y = lax.axis_index("cb")
    twin = 1 - y
    rows = xa.shape[3]
    half = xa.shape[4]
    model_width = 2 * n * half
    up_cols = wu.shape[1]
    steps = wu.shape[0] // STEP_ROWS

    def load(ref, i, slot):
        return pltpu.make_async_copy(
            ref.at[pl.ds(i * STEP_ROWS, STEP_ROWS)], stage.at[slot], load_sem.at[slot]
        )

    for i in range(SLOTS):
        load(wu_ref, i, i).start()

    def own_piece(c, h):
        return pltpu.make_async_copy(
            x_ref.at[pl.ds(c * rows, rows), pl.ds(h * half, half)],
            xa.at[c, z, h],
            own_sem.at[c, h],
        )

    for c in range(chunks):
        for h in range(2):
            own_piece(c, h).start()

    barrier = pltpu.get_barrier_semaphore()
    for j in range(1, n):
        pl.semaphore_signal(
            barrier, inc=1, device_id={"ra": lax.rem(z + j, n)}, device_id_type=MESH
        )
    pl.semaphore_signal(barrier, inc=1, device_id={"cb": twin}, device_id_type=MESH)
    pl.semaphore_wait(barrier, n)

    def remote(src, dst, send, recv, where):
        return pltpu.make_async_remote_copy(
            src_ref=src, dst_ref=dst, send_sem=send, recv_sem=recv,
            device_id=where, device_id_type=MESH,
        )

    def x_copy(c, src, way):
        piece = xa.at[c, src, y]
        return remote(piece, piece, xs.at[c, src, way], xr.at[c, src], {"ra": z + 1 - 2 * way})

    def y_copy(c, src):
        piece = xa.at[c, src, y]
        return remote(piece, piece, ys.at[c, src], yr.at[c, src], {"cb": twin})

    def y_arrive(c, src):
        piece = xa.at[c, src, twin]
        return remote(piece, piece, ys.at[c, src], yr.at[c, src], {"cb": twin})

    def d_copy(c, src, way):
        piece = down.at[c, src]
        return remote(piece, piece, fs.at[c, src, way], fr.at[c, src], {"ra": z + 1 - 2 * way})

    def start_line(copy, c):
        @pl.when(z + 1 < n)
        def _():
            copy(c, z, 0).start()

        @pl.when(z > 0)
        def _():
            copy(c, z, 1).start()

    def relay(copy, c, k, also=None):
        @pl.when(z - k >= 0)
        def _():
            src = z - k
            copy(c, src, 0).wait_recv()

            @pl.when(z + 1 < n)
            def _():
                copy(c, src, 0).start()

            if also is not None:
                also(c, src).start()

        @pl.when(z + k < n)
        def _():
            src = z + k
            copy(c, src, 1).wait_recv()

            @pl.when(z > 0)
            def _():
                copy(c, src, 1).start()

            if also is not None:
                also(c, src).start()

    def gain_copy(where, src):
        return remote(gain_ref, gains.at[src], gs.at[where], gr.at[src], {"ra": where})

    def begin(c):
        if c < chunks:
            for h in range(2):
                own_piece(c, h).wait()
            start_line(x_copy, c)

    begin(0)
    for j in range(1, n):
        gain_copy(lax.rem(z + j, n), z).start()
    gains[z] = gain_ref[...]
    begin(1)

    def gather_step(c, k):
        relay(x_copy, c, k, y_copy)
        if k == 1:
            begin(c + 2)

    def convert(ref, target, following, lo, hi):
        def body(i, carry):
            slot = lax.rem(i + (0 if following is not None else steps), SLOTS)
            load(ref, i, slot).wait()
            target[pl.ds(pl.multiple_of(i * STEP_ROWS, STEP_ROWS), STEP_ROWS), :] = stage[
                slot
            ].astype(jnp.bfloat16)

            @pl.when(i + SLOTS < steps)
            def _():
                load(ref, i + SLOTS, slot).start()

            if following is not None:
                @pl.when(i + SLOTS >= steps)
                def _():
                    load(following, i + SLOTS - steps, slot).start()

            return carry

        lax.fori_loop(lo, hi, body, 0)

    def convert_with_gather(ref, target, following, among):
        relays = [(c, k) for c in among if c < chunks for k in range(1, n)]
        cuts = [steps * k // (len(relays) + 1) for k in range(len(relays) + 2)]
        for i in range(len(relays) + 1):
            convert(ref, target, following, cuts[i], cuts[i + 1])
            if i < len(relays):
                gather_step(*relays[i])

    def hid_copy(c, block):
        piece = hid.at[c, block]
        return remote(piece, piece, hs.at[c], hr.at[c], {"cb": twin})

    def up(c):
        for j in range(1, n):
            y_arrive(c, lax.rem(z + j, n)).wait_recv()
        total = jnp.zeros((rows, 1), jnp.float32)
        for s in range(n):
            for h in range(2):
                xf = xa[c, s, h].astype(jnp.float32)
                total += jnp.sum(xf * xf, axis=1, keepdims=True)
                gain = gains[s][:, h * half : (h + 1) * half]
                lo = (2 * s + h) * half
                normed[:, lo : lo + half] = (xf * gain).astype(jnp.bfloat16)
        inv_in = lax.rsqrt(total / model_width + epsilon)
        tile = 256

        def body(j, carry):
            cols = pl.ds(pl.multiple_of(j * tile, tile), tile)
            pre = jnp.dot(normed[...], wu[:, cols], preferred_element_type=jnp.float32)
            pre = jnp.maximum(pre * inv_in * us_ref[:, cols], 0.0)
            hid[c, y, :, cols] = (pre * pre).astype(jnp.bfloat16)
            return carry

        lax.fori_loop(0, up_cols // tile, body, 0)
        hid_copy(c, y).start()

    def part_copy(c, where, src):
        return remote(
            parts.at[c, where], rbuf.at[c, src], rs.at[c, where], rr.at[c, src], {"ra": where}
        )

    def down_product(c):
        hid_copy(c, twin).wait_recv()

        def body(q, carry):
            cols = pl.ds(pl.multiple_of(q * half, half), half)
            acc = jnp.dot(hid[c, 0], wd[:up_cols, cols], preferred_element_type=jnp.float32)
            acc += jnp.dot(hid[c, 1], wd[up_cols:, cols], preferred_element_type=jnp.float32)
            parts[c, q] = acc.astype(jnp.bfloat16)
            return carry

        lax.fori_loop(0, n, body, 0)
        for j in range(1, n):
            part_copy(c, lax.rem(z + j, n), z).start()

    def reduce(c):
        acc = parts[c, z].astype(jnp.float32)
        for j in range(1, n):
            src = lax.rem(z + j, n)
            part_copy(c, src, src).wait_recv()
            acc += rbuf[c, src].astype(jnp.float32)
        down[c, z] = acc.astype(jnp.bfloat16)
        start_line(d_copy, c)

    def sq_copy(c):
        return remote(sq.at[c], sqr.at[c], qs.at[c], qr.at[c], {"cb": twin})

    def mix(c):
        total = jnp.zeros((rows, 1), jnp.float32)
        for q in range(n):
            cols = slice(q * half, (q + 1) * half)
            at = y * n + q
            resid = xa[c, at // 2, at % 2].astype(jnp.float32)
            value = resid_weight * resid + down[c, q].astype(jnp.float32) * ds_ref[:, cols]
            mixed[c % 2, :, cols] = value
            total += jnp.sum(value * value, axis=1, keepdims=True)
        sq[c] = jnp.broadcast_to(total, (rows, 128))
        sq_copy(c).start()

    def finish(c):
        sq_copy(c).wait_recv()
        total = sq[c][:, :1] + sqr[c][:, :1]
        inv_out = lax.rsqrt(total / model_width + epsilon)
        o_ref[c * rows : (c + 1) * rows, :] = (mixed[c % 2] * inv_out * no_ref[...]).astype(
            jnp.bfloat16
        )

    convert_with_gather(wu_ref, wu, wd_ref, (0,))
    for j in range(1, n):
        src = lax.rem(z + j, n)
        gain_copy(src, src).wait_recv()
    up(0)
    convert_with_gather(wd_ref, wd, None, (1, 2))
    def spread(c, lo, hi):
        if 0 <= c < chunks:
            for k in range(lo, hi):
                relay(d_copy, c, k)

    for t in range(1, chunks + 4):
        if t < chunks:
            up(t)
        spread(t - 3, 1, 2)
        if 0 <= t - 1 < chunks:
            down_product(t - 1)
        spread(t - 3, 2, n)
        if 2 < t + 2 < chunks:
            for k in range(1, n):
                gather_step(t + 2, k)
        if 0 <= t - 2 < chunks:
            reduce(t - 2)
        if 0 <= t - 4 < chunks:
            finish(t - 4)
        if 0 <= t - 3 < chunks:
            mix(t - 3)

    for j in range(1, n):
        gain_copy(lax.rem(z + j, n), z).wait_send()

    def drain(c, carry):
        for src in range(n):
            @pl.when((src <= z) & (z + 1 < n))
            def _():
                x_copy(c, src, 0).wait_send()
                d_copy(c, src, 0).wait_send()

            @pl.when((src >= z) & (z > 0))
            def _():
                x_copy(c, src, 1).wait_send()
                d_copy(c, src, 1).wait_send()

            @pl.when(z != src)
            def _():
                y_copy(c, src).wait_send()
                part_copy(c, src, z).wait_send()

        hid_copy(c, y).wait_send()
        sq_copy(c).wait_send()
        return carry

    lax.fori_loop(0, chunks, drain, 0)


def fused(n, tokens, norm_in, w_up, up_scale, w_down, down_scale, norm_out):
    chunks = CHUNKS
    rows = tokens.shape[0] // chunks
    half = tokens.shape[1] // 2
    wide = w_down.shape[1]
    bf16, f32 = jnp.bfloat16, jnp.float32
    dma = pltpu.SemaphoreType.DMA
    vmem = pl.BlockSpec(memory_space=pltpu.VMEM)
    far = pl.BlockSpec(memory_space=pl.ANY)
    flops = 2 * tokens.shape[0] * (w_up.size + w_down.size)
    return pl.pallas_call(
        functools.partial(kernel, n, chunks),
        out_shape=jax.ShapeDtypeStruct((tokens.shape[0], wide), bf16),
        in_specs=[far, vmem, far, vmem, far, vmem, vmem],
        out_specs=vmem,
        scratch_shapes=[
            pltpu.VMEM((chunks, n, 2, rows, half), bf16),
            pltpu.VMEM((n, 1, 2 * half), f32),
            pltpu.VMEM(w_up.shape, bf16),
            pltpu.VMEM(w_down.shape, bf16),
            pltpu.VMEM((SLOTS, STEP_ROWS, wide), f32),
            pltpu.VMEM((rows, 2 * half * n), bf16),
            pltpu.VMEM((chunks, 2, rows, w_up.shape[1]), bf16),
            pltpu.VMEM((chunks, n, rows, half), bf16),
            pltpu.VMEM((chunks, n, rows, half), bf16),
            pltpu.VMEM((chunks, n, rows, half), bf16),
            pltpu.VMEM((2, rows, wide), f32),
            pltpu.VMEM((chunks, rows, 128), f32),
            pltpu.VMEM((chunks, rows, 128), f32),
            dma((SLOTS,)),
            dma((chunks, 2)),
            dma((n,)),
            dma((n,)),
            dma((chunks, n, 2)),
            dma((chunks, n)),
            dma((chunks, n)),
            dma((chunks, n)),
            dma((chunks,)),
            dma((chunks,)),
            dma((chunks, n)),
            dma((chunks, n)),
            dma((chunks, n, 2)),
            dma((chunks, n)),
            dma((chunks,)),
            dma((chunks,)),
        ],
        compiler_params=pltpu.CompilerParams(
            collective_id=0, has_side_effects=True, vmem_limit_bytes=67043328
        ),
        cost_estimate=pl.CostEstimate(
            flops=flops, bytes_accessed=4 * (w_up.size + w_down.size), transcendentals=0
        ),
    )(
        tokens,
        norm_in.astype(f32)[None, :],
        w_up,
        up_scale[None, :],
        w_down,
        down_scale[None, :],
        norm_out[None, :],
    )


def solution(mesh):
    n, m = mesh.shape["ra"], mesh.shape["cb"]

    def per_device(tokens, norm_in, w_up, up_scale, w_down, down_scale, norm_out):
        args = (tokens, norm_in, w_up, up_scale, w_down, down_scale, norm_out)
        fits = (
            m == 2
            and n > 1
            and CHUNKS > 1
            and tokens.shape[0] % (CHUNKS * 16) == 0
            and tokens.shape[1] % 256 == 0
            and w_up.shape == w_down.shape
            and w_up.shape[0] % (STEP_ROWS * n) == 0
            and w_up.shape[0] // STEP_ROWS >= SLOTS
            and w_up.shape[1] % 256 == 0
            and w_up.size <= 8 * 1024 * 1024
            and tokens.size * n <= 2 * 1024 * 1024
        )
        return fused(n, *args) if fits else plain(*args)

    placed = (
        P("dp", "ra"),
        P("ra"),
        P(None, ("ra", "cb")),
        P(("ra", "cb")),
        P("ra", "cb"),
        P("cb"),
        P("cb"),
    )
    return jax.shard_map(
        per_device, mesh=mesh, in_specs=placed, out_specs=P("dp", "cb"), check_vma=False
    )
```
